32 devices in a mesh: sp: 4 (over y, x), tp: 8 (over z, core).
Axes of the slice: x: 2, y: 2, z: 4, core: 2. Of those that a mesh axis runs over, the one named last changes fastest.
Arguments:
- prompt: bfloat16 [2, 8, 2, 4, 128, 2048], P(None, 'tp', None, 'sp'), may hold values from -60 to 60
- new_token: bfloat16 [2, 2048], replicated, may hold values from -20 to 20
- query_proj_matrix: bfloat16 [2048, 1024], P(None, 'tp'), may hold values from -1 to 1
- key_weight: bfloat16 [2048, 1024], P(None, 'tp'), may hold values from -1 to 1
- value_weight: bfloat16 [2048, 1024], P(None, 'tp'), may hold values from -0.125 to 0.125
- map_balance: float32 [8], replicated, may hold values from 0.3 to 0.8
- head_gain: float32 [128], replicated, may hold values from 0.1 to 1.9
Outputs:
- key_cache: bfloat16 [4, 8, 512, 1024], P('sp', 'tp')
- value_cache: bfloat16 [4, 8, 512, 1024], P('sp', 'tp')
- read: float32 [2, 1024], replicated
The draws below stay inside these ranges and needn't reach their ends.
All inputs are finite; a program needn't handle non-finite values.
Results may differ from the reference program's by a relative error of at most 0.004.
The reference program's roundings to bfloat16 on the way (of `queries`) count: a program that leaves them out, or rounds other values in their place, can miss the bound.
Values may be sent and summed in bfloat16 or wider, within the bound.
A program may use at most 64 MiB of HBM per device.

```python
import math
import jax
import jax.numpy as jnp
from jax import lax

D = 2048
HEADS = 8
MAP_HEAD_SIZE = 64
VD = 128
SEQS = 2
KW = 1024
VW = 1024
GROUP = 2
SUB = 128
TILES = 8
SPAN = 512
LEN = 8192
N_SP = 4


def shared_query(key):
    base = jax.random.normal(jax.random.fold_in(key, 11), (D, KW), jnp.float32)
    return jnp.clip(base, -6.0, 6.0) / math.sqrt(D)


def shared_new(key):
    base = jnp.clip(jax.random.normal(jax.random.fold_in(key, 13), (SEQS, D), jnp.float32), -6.0, 6.0) * 1.3
    return base


def draw_query_proj_matrix(key, part):
    return shared_query(key).astype(jnp.bfloat16)


def draw_key_weight(key, part):
    base = jax.random.normal(jax.random.fold_in(key, 12), (D, KW), jnp.float32)
    own = jnp.clip(base, -6.0, 6.0) / math.sqrt(D)
    matrix = own
    return matrix.astype(jnp.bfloat16)


def draw_new_token(key, part):
    return shared_new(key).astype(jnp.bfloat16)


def draw_prompt(key, part):
    base = jax.random.normal(jax.random.fold_in(key, 14), (SEQS, LEN, D), jnp.float32)
    base = jnp.clip(base, -6.0, 6.0) * 1.3
    return base.reshape(SEQS, TILES, GROUP, N_SP, SUB, D).astype(jnp.bfloat16)


def block_levels(rng, shape, pieces, smallest, top_value):
    loudness = 1.0
    for axis_at, blocks in pieces:
        draws = jax.random.uniform(jax.random.fold_in(jax.random.fold_in(rng, 6), axis_at), (blocks,), jnp.float32, smallest / len(pieces), top_value / len(pieces))
        loudness = loudness * jnp.repeat(jnp.exp(draws), shape[axis_at] // blocks).reshape((-1,) + (1,) * (len(shape) - 1 - axis_at))
    return loudness


def normal_values(stream_key, dims, spread, reach, pieces=(), held_as=jnp.bfloat16):
    result = spread * jax.random.normal(stream_key, dims, jnp.float32)
    if pieces:
        result = result * block_levels(stream_key, dims, pieces, -0.22, 0.18)
    return jnp.clip(result, -reach, reach).astype(held_as)


def setup_inputs(seed: int = 0) -> dict:
    splits = jax.random.split(jax.random.key(seed), 8)
    return {
        "prompt": draw_prompt(jax.random.fold_in(splits[7], 71), 0),
        "new_token": draw_new_token(jax.random.fold_in(splits[7], 71), 0),
        "query_proj_matrix": draw_query_proj_matrix(jax.random.fold_in(splits[7], 71), 0),
        "key_weight": draw_key_weight(jax.random.fold_in(splits[7], 71), 0),
        "value_weight": normal_values(splits[4], (D, VW), D ** -0.5, 0.125, ((1, 8),)),
        "map_balance": jnp.clip(jax.random.uniform(splits[5], (HEADS,), jnp.float32, 0.3, 0.8), 0.3, 0.8),
        "head_gain": jnp.clip(1.0 + 0.18 * jax.random.normal(splits[6], (VD,), jnp.float32), 0.1, 1.9),
    }


norm_eps = 1e-06

def project(inputs, weight_matrix):
    return jnp.dot(inputs, weight_matrix, preferred_element_type=jnp.float32).astype(jnp.bfloat16)

def relayout(rows, width):
    shaped = rows.reshape(SEQS, TILES, GROUP, SPAN, width)
    return jnp.transpose(shaped, (0, 2, 1, 3, 4)).reshape(SEQS * GROUP, TILES, SPAN, width)

def reference(prompt, new_token, query_proj_matrix, key_weight, value_weight, map_balance, head_gain):

    def cache_rows(sequence):
        flat_rows = sequence.reshape(LEN, D)
        return (project(flat_rows, key_weight), project(flat_rows, value_weight))
    flat_keys, flat_values = lax.map(cache_rows, prompt)
    queries = project(new_token, query_proj_matrix)
    new_keys = project(new_token, key_weight)
    new_values = project(new_token, value_weight)

    def read_one(inputs):
        seq_keys, seq_values, own_query, own_key, own_value = inputs
        every_key_row = jnp.concatenate([seq_keys, own_key[None, :]], axis=0)
        every_key_row = every_key_row.astype(jnp.float32).reshape(LEN + 1, HEADS, 2, MAP_HEAD_SIZE)
        all_values = jnp.concatenate([seq_values, own_value[None, :]], axis=0)
        all_values = all_values.astype(jnp.float32).reshape(LEN + 1, HEADS, VD)
        query_matrix_rows = own_query.astype(jnp.float32).reshape(HEADS, 2, MAP_HEAD_SIZE)
        logit_scores = jnp.einsum('rkx,vrkx->rkv', query_matrix_rows, every_key_row) * MAP_HEAD_SIZE ** (-0.5)
        probs = jax.nn.softmax(logit_scores, axis=-1)
        heads_out = jnp.einsum('hmj,jhe->hme', probs, all_values)
        blended = heads_out[:, 0] - map_balance[:, None] * heads_out[:, 1]
        normed = blended * lax.rsqrt(lax.optimization_barrier(jnp.mean(blended * blended, axis=-1, keepdims=True)) + norm_eps) * head_gain
        return normed.reshape(HEADS * VD)
    read = lax.map(read_one, (flat_keys, flat_values, queries, new_keys, new_values))
    return (relayout(flat_keys, KW), relayout(flat_values, VW), read)
```

```python
import functools

import jax
import jax.numpy as jnp
from jax import lax
from jax.experimental import pallas as pl
from jax.experimental.pallas import tpu as pltpu
from jax.sharding import PartitionSpec as P

HEADS = 8
MAP_HEAD_SIZE = 64
VD = 128


norm_eps = 1e-06
far_below = -1e30


def joined(part, axis, combine):
    gathered = jax.tree.map(lambda a: lax.all_gather(a, axis), part)

    def take(source):
        return jax.tree.map(lambda a: lax.dynamic_index_in_dim(a, source, 0, False), gathered)

    return lax.fori_loop(
        1, lax.axis_size(axis), lambda source, state: combine(state, take(source)), take(0)
    )


def fill_cols(source, w_piece):
    product = jnp.dot(source, w_piece, preferred_element_type=jnp.float32).astype(jnp.bfloat16)
    return product


def local_new(new_token, query_proj_matrix, key_weight, value_weight):
    return (
        jnp.dot(new_token, query_proj_matrix, preferred_element_type=jnp.float32).astype(
            jnp.bfloat16
        ),
        jnp.dot(new_token, key_weight, preferred_element_type=jnp.float32).astype(jnp.bfloat16),
        jnp.dot(new_token, value_weight, preferred_element_type=jnp.float32).astype(jnp.bfloat16),
    )


def partial_read(query_matrix_rows, key_rows, value_rows):
    logit_scores = jnp.einsum(
        "bhmd,bjhmd->bhmj", query_matrix_rows, key_rows, preferred_element_type=jnp.float32
    ) * MAP_HEAD_SIZE ** (-0.5)
    peak = jnp.max(logit_scores, axis=-1)
    weights_exp = jnp.exp(logit_scores - peak[..., None])
    totals = jnp.sum(weights_exp, axis=-1)
    weighted = jnp.einsum("bhmj,bjhe->bhme", weights_exp, value_rows.astype(jnp.float32))
    return (peak, totals, weighted)


def combine(first, second):
    peak_a, totals_a, weighted_a = first
    peak_b, totals_b, weighted_b = second
    peak = jnp.maximum(peak_a, peak_b)
    factor_a = jnp.exp(peak_a - peak)
    factor_b = jnp.exp(peak_b - peak)
    return (
        peak,
        totals_a * factor_a + totals_b * factor_b,
        weighted_a * factor_a[..., None] + weighted_b * factor_b[..., None],
    )


def shards(prompt, new_token, query_proj_matrix, key_weight, value_weight, map_balance, head_gain):
    seq_count, _, span_count, _, piece_rows, model_width = prompt.shape
    token_rows = prompt.reshape(seq_count * span_count * piece_rows, model_width)
    tp_count = lax.axis_size("tp")
    key_width = key_weight.shape[1] * tp_count
    value_width = value_weight.shape[1] * tp_count
    key_piece = lax.all_gather(key_weight, "tp", axis=1, tiled=True)
    value_piece = lax.all_gather(value_weight, "tp", axis=1, tiled=True)
    key_rows = fill_cols(token_rows, key_piece)
    value_rows = fill_cols(token_rows, value_piece)
    own_columns = local_new(new_token, query_proj_matrix, key_weight, value_weight)
    queries, new_keys, new_values = (
        lax.all_gather(own_columns[0], "tp", axis=1, tiled=True),
        lax.all_gather(own_columns[1], "tp", axis=1, tiled=True),
        lax.all_gather(own_columns[2], "tp", axis=1, tiled=True),
    )
    slot_count = seq_count * span_count
    cached_keys, cached_values = (
        lax.all_to_all(
            key_rows.reshape(slot_count, piece_rows, key_width),
            "sp",
            split_axis=0,
            concat_axis=1,
            tiled=True,
        ),
        lax.all_to_all(
            value_rows.reshape(slot_count, piece_rows, value_width),
            "sp",
            split_axis=0,
            concat_axis=1,
            tiled=True,
        ),
    )
    block_rows = cached_keys.shape[1]
    key_cache = cached_keys.reshape(1, 1, block_rows, key_width)
    value_cache = cached_values.reshape(1, 1, block_rows, value_width)
    all_queries = queries.reshape(seq_count, HEADS, 2, MAP_HEAD_SIZE)
    own_seq = lax.axis_index("sp") // span_count
    own_query = lax.dynamic_slice_in_dim(all_queries, own_seq, 1, 0)
    peak, totals, weighted = partial_read(
        own_query,
        cached_keys.reshape(1, block_rows, HEADS, 2, MAP_HEAD_SIZE),
        cached_values.reshape(1, block_rows, HEADS, VD),
    )
    chosen = jnp.arange(seq_count) == own_seq
    chosen_rows = chosen[:, None, None]
    spread = (
        jnp.where(chosen_rows, peak, far_below),
        jnp.where(chosen_rows, totals, 0.0),
        jnp.where(chosen_rows[..., None], weighted, 0.0),
    )
    merged = joined(spread, ("sp", "tp"), combine)
    own_keys = new_keys.reshape(seq_count, HEADS, 2, MAP_HEAD_SIZE)
    own_score = jnp.einsum(
        "bhmd,bhmd->bhm", all_queries, own_keys, preferred_element_type=jnp.float32
    ) * MAP_HEAD_SIZE ** (-0.5)
    own_values = new_values.astype(jnp.float32).reshape(seq_count, HEADS, VD)
    own_weighted = jnp.broadcast_to(own_values[:, :, None, :], (seq_count, HEADS, 2, VD))
    own_state = (own_score, jnp.ones_like(own_score), own_weighted)
    _, totals, weighted = combine(merged, own_state)
    heads_out = weighted / totals[..., None]
    blended = heads_out[:, :, 0] - map_balance[None, :, None] * heads_out[:, :, 1]
    normed = (
        blended
        * lax.rsqrt(jnp.mean(blended * blended, axis=-1, keepdims=True) + norm_eps)
        * head_gain
    )
    return (key_cache, value_cache, normed.reshape(seq_count, HEADS * VD))


MESH = pl.DeviceIdType.MESH
CORES = 2


def merged_states(states):
    half = VD // 2
    peaks = [a[:, VD : VD + 1] for a in states]
    totals = [a[:, VD + half : VD + half + 1] for a in states]
    peak = functools.reduce(jnp.maximum, peaks)
    factors = [jnp.exp(p - peak) for p in peaks]
    total = functools.reduce(jnp.add, [t * f for t, f in zip(totals, factors)])
    weighted = functools.reduce(jnp.add, [a[:, :VD] * f for a, f in zip(states, factors)])
    return weighted, peak, total


def packed_state(weighted, peak, total):
    lane = lax.broadcasted_iota(jnp.int32, weighted.shape, 1)
    tail = jnp.where(lane < VD // 2, peak, total)
    return jnp.concatenate([weighted, tail], axis=1)


def step_kernel(
    dims,
    prompt, token, wq_hbm, wk_hbm, wv_hbm, balance, gain,
    kout, vout, read,
    xbuf, wbuf, wq, qbuf, own, stbuf, finbuf,
    loc, pr_send, pr_recv, line_send, prim_recv, sib_send, sib_recv, xy_send, sec_recv,
    pk_send, pk_recv, st_send, st_recv, fin_send, fin_recv,
):
    sp_count, tp_count, seq_count = dims
    depth = wbuf.shape[2]
    cols = wbuf.shape[3] // CORES
    chips = tp_count // CORES
    s = lax.axis_index("sp")
    t = lax.axis_index("tp")
    z = t // CORES
    c = t % CORES
    sib = z * CORES + (1 - c)
    xs = s + 1 - 2 * (s % 2)
    ys = (s + 2) % 4
    prim = (s + s // 2) % 2
    sec = 1 - prim
    lanes = pl.ds(pl.multiple_of(c * cols, cols), cols)
    half = depth // 2

    loads = [
        pltpu.make_async_copy(wk_hbm, wbuf.at[0, z, :, lanes], loc.at[0]),
        pltpu.make_async_copy(wv_hbm, wbuf.at[1, z, :, lanes], loc.at[1]),
        pltpu.make_async_copy(wq_hbm, wq, loc.at[2]),
        pltpu.make_async_copy(prompt.at[s], xbuf.at[s], loc.at[3]),
    ]
    for a in loads:
        a.start()

    barrier = pltpu.get_barrier_semaphore()
    for d in range(1, sp_count):
        pl.semaphore_signal(barrier, inc=1, device_id=((s + d) % sp_count, t), device_id_type=MESH)
    for d in range(1, tp_count):
        pl.semaphore_signal(barrier, inc=1, device_id=(s, (t + d) % tp_count), device_id_type=MESH)
    pl.semaphore_wait(barrier, sp_count + tp_count - 2)

    def remote(src, dst, send, recv, dev):
        return pltpu.make_async_remote_copy(
            src_ref=src, dst_ref=dst, send_sem=send, recv_sem=recv, device_id=dev, device_id_type=MESH
        )

    def block(m, zz):
        return wbuf.at[m, zz, :, lanes]

    def part(m, zz, h):
        return wbuf.at[m, zz, pl.ds(h * half, half), lanes]

    sends = []

    def go(copy):
        copy.start()
        sends.append(copy)

    loads[0].wait()
    loads[1].wait()

    def line(direction, zz):
        return remote(
            block(prim, zz), block(prim, zz), line_send.at[(direction + 1) // 2, zz], prim_recv.at[zz],
            (s, t + direction * CORES),
        )

    def has_next(direction):
        return (z > 0) if direction < 0 else (z < chips - 1)

    for direction in (-1, 1):
        pl.when(has_next(direction))(lambda direction=direction: line(direction, z).start())
    for d in (1, 2, 3):
        p = xs if d == 1 else ys if d == 2 else 3 - s
        go(remote(prompt.at[p], xbuf.at[s], pr_send.at[d], pr_recv.at[s], (p, t)))
    for m in range(2):
        go(remote(block(m, z), block(m, z), sib_send.at[m, z, 0], sib_recv.at[m, z, 0], (s, sib)))

    loads[2].wait()
    rows = token[...]
    me_q = jnp.dot(rows, wq[...], preferred_element_type=jnp.float32)
    me_k = jnp.dot(rows, wbuf[0, z, :, lanes], preferred_element_type=jnp.float32)
    me_v = jnp.dot(rows, wbuf[1, z, :, lanes], preferred_element_type=jnp.float32)
    for i, value in enumerate((me_q, me_k, me_v)):
        value = value.astype(jnp.bfloat16).astype(jnp.float32)
        qbuf[t, i * seq_count : (i + 1) * seq_count, :] = value[:seq_count]
    for d in range(1, tp_count):
        go(remote(qbuf.at[t], qbuf.at[t], pk_send.at[d], pk_recv.at[t], (s, (t + d) % tp_count)))

    near = jnp.minimum(z, chips - 1 - z)

    def source(j):
        paired = j <= 2 * near
        dist = jnp.where(paired, (j + 1) // 2, j - near)
        from_left = jnp.where(paired, j % 2 == 1, z > near)
        return jnp.where(from_left, z - dist, z + dist), from_left

    sources = [source(j) for j in range(1, chips)]

    def forwards(from_left):
        return (
            jnp.logical_and(from_left, z < chips - 1),
            jnp.logical_and(jnp.logical_not(from_left), z > 0),
        )

    def arrive_primary(j):
        zz, from_left = sources[j]
        remote(block(prim, zz), block(prim, zz), line_send.at[0, zz], prim_recv.at[zz], (s, t)).wait_recv()
        for on, direction in zip(forwards(from_left), (1, -1)):
            pl.when(on)(lambda direction=direction: line(direction, zz).start())
        go(remote(part(prim, zz, 0), part(prim, zz, 0), xy_send.at[0, zz], sec_recv.at[0, zz], (xs, t)))
        go(remote(part(prim, zz, 1), part(prim, zz, 1), xy_send.at[1, zz], sec_recv.at[1, zz], (ys, t)))
        go(remote(block(prim, zz), block(prim, zz), sib_send.at[0, zz, 0], sib_recv.at[0, zz, 0], (s, sib)))

    def arrive_secondary(j):
        zz, _ = sources[j]
        for h in range(2):
            remote(part(sec, zz, h), part(sec, zz, h), xy_send.at[h, zz], sec_recv.at[h, zz], (s, t)).wait_recv()
            go(remote(part(sec, zz, h), part(sec, zz, h), sib_send.at[1, zz, h], sib_recv.at[1, zz, h], (s, sib)))

    sib_lanes = pl.ds(pl.multiple_of((1 - c) * cols, cols), cols)

    def wait_sibling(m, slot, zz, h):
        view = wbuf.at[m, zz, :, sib_lanes] if h is None else wbuf.at[m, zz, pl.ds(h * half, half), sib_lanes]
        h = 0 if h is None else h
        remote(view, view, sib_send.at[slot, zz, h], sib_recv.at[slot, zz, h], (s, t)).wait_recv()

    def multiply(m, zz):
        weights = wbuf.at[m, zz]
        columns = pl.ds(pl.multiple_of(zz * CORES * cols, CORES * cols), CORES * cols)

        def piece(i, _):
            product = jnp.dot(
                xbuf[pl.ds(2 * i, 2)].reshape(-1, depth), weights[...], preferred_element_type=jnp.float32
            ).astype(jnp.bfloat16)
            at = pl.ds(pl.multiple_of(i * product.shape[0], product.shape[0]), product.shape[0])

            def put(out):
                out[at, columns] = product

            if isinstance(m, int):
                put((kout, vout)[m])
            else:
                pl.when(m == 0)(lambda: put(kout))
                pl.when(m == 1)(lambda: put(vout))
            return 0

        lax.fori_loop(0, sp_count // 2, piece, 0)

    def multiply_primary(j):
        zz, _ = sources[j]
        wait_sibling(prim, 0, zz, None)
        multiply(prim, zz)

    def multiply_secondary(j):
        zz, _ = sources[j]
        for h in range(2):
            wait_sibling(sec, 1, zz, h)
        multiply(sec, zz)

    last = chips - 1
    for j in range(min(2, last)):
        arrive_primary(j)

    for d in range(1, tp_count):
        i = (t + d) % tp_count
        remote(qbuf.at[i], qbuf.at[i], pk_send.at[d], pk_recv.at[i], (s, t)).wait_recv()
    new = jnp.concatenate([qbuf[i] for i in range(tp_count)], axis=1)
    row = lax.broadcasted_iota(jnp.int32, (2 * HEADS, new.shape[1]), 0)
    lane = lax.broadcasted_iota(jnp.int32, (2 * HEADS, new.shape[1]), 1)
    own_lane = lane // MAP_HEAD_SIZE == (row % HEADS) * 2 + row // HEADS
    scale = MAP_HEAD_SIZE ** (-0.5)
    short_row = lax.broadcasted_iota(jnp.int32, (2 * HEADS, VD), 0) % HEADS

    def by_head(wide):
        return functools.reduce(
            jnp.add,
            [jnp.where(short_row == h, wide[:, h * VD : (h + 1) * VD], 0.0) for h in range(HEADS)],
        )

    own_seq = s // (sp_count // seq_count)
    query = jnp.zeros((2 * HEADS, new.shape[1]), jnp.float32)
    for b in range(seq_count):
        q_b = jnp.broadcast_to(new[b : b + 1], query.shape)
        k_b = jnp.broadcast_to(new[seq_count + b : seq_count + b + 1], query.shape)
        v_b = jnp.broadcast_to(new[2 * seq_count + b : 2 * seq_count + b + 1], query.shape)
        score = jnp.sum(jnp.where(own_lane, q_b * k_b, 0.0), axis=1, keepdims=True) * scale
        own[b] = packed_state(by_head(v_b), score, jnp.ones_like(score))
        query = jnp.where(own_seq == b, q_b, query)
    query = jnp.where(own_lane, query, 0.0).astype(jnp.bfloat16)

    loads[3].wait()
    for d, p in ((1, xs), (2, ys), (3, 3 - s)):
        remote(xbuf.at[p], xbuf.at[p], pr_send.at[d], pr_recv.at[p], (s, t)).wait_recv()
    for m in range(2):
        wait_sibling(m, m, z, None)
        multiply(m, z)
    for j in range(last):
        if j >= 2:
            arrive_primary(j)
        multiply_primary(j)
        if j >= 1:
            arrive_secondary(j - 1)
            multiply_secondary(j - 1)
    arrive_secondary(last - 1)
    multiply_secondary(last - 1)

    scores = lax.dot_general(
        query, kout[...], (((1,), (1,)), ((), ())), preferred_element_type=jnp.float32
    ) * scale
    peak = jnp.max(scores, axis=1, keepdims=True)
    raised = jnp.exp(scores - peak)
    total = jnp.sum(raised, axis=1, keepdims=True)
    high = raised.astype(jnp.bfloat16)
    low = (raised - high.astype(jnp.float32)).astype(jnp.bfloat16)
    wide = jnp.dot(high, vout[...], preferred_element_type=jnp.float32)
    wide = wide + jnp.dot(low, vout[...], preferred_element_type=jnp.float32)
    stbuf[t] = packed_state(by_head(wide), peak, total)
    for d in range(1, tp_count):
        go(remote(stbuf.at[t], stbuf.at[t], st_send.at[d], st_recv.at[t], (s, (t + d) % tp_count)))
    for d in range(1, tp_count):
        i = (t + d) % tp_count
        remote(stbuf.at[i], stbuf.at[i], st_send.at[d], st_recv.at[i], (s, t)).wait_recv()
    finbuf[s] = packed_state(*merged_states([stbuf[i] for i in range(tp_count)]))
    for d in range(1, sp_count):
        go(remote(finbuf.at[s], finbuf.at[s], fin_send.at[d], fin_recv.at[s], ((s + d) % sp_count, t)))
    for d in range(1, sp_count):
        i = (s + d) % sp_count
        remote(finbuf.at[i], finbuf.at[i], fin_send.at[d], fin_recv.at[i], (s, t)).wait_recv()
    spans = sp_count // seq_count
    for b in range(seq_count):
        weighted, _, total = merged_states([finbuf[b * spans + i] for i in range(spans)] + [own[b]])
        heads_out = weighted / total
        blended = heads_out[:HEADS] - balance[...] * heads_out[HEADS:]
        normed = (
            blended * lax.rsqrt(jnp.mean(blended * blended, axis=1, keepdims=True) + norm_eps) * gain[...]
        )
        for h in range(HEADS):
            read[b : b + 1, h * VD : (h + 1) * VD] = normed[h : h + 1]

    for direction in (-1, 1):
        pl.when(has_next(direction))(lambda direction=direction: line(direction, z).wait_send())
    for zz, from_left in sources:
        for on, direction in zip(forwards(from_left), (1, -1)):
            pl.when(on)(lambda direction=direction, zz=zz: line(direction, zz).wait_send())
    for copy in sends:
        copy.wait_send()


def fused(prompt, new_token, query_proj_matrix, key_weight, value_weight, map_balance, head_gain):
    seq_count, _, span_count, _, piece_rows, width = prompt.shape
    sp_count, tp_count = lax.axis_size("sp"), lax.axis_size("tp")
    cols = key_weight.shape[1]
    slots = seq_count * span_count
    chips = tp_count // CORES
    key_width = cols * tp_count
    block_rows = sp_count * piece_rows
    any_space = pl.BlockSpec(memory_space=pl.ANY)
    vmem = pl.BlockSpec(memory_space=pltpu.VMEM)
    dma = pltpu.SemaphoreType.DMA
    keys, values, read = pl.pallas_call(
        functools.partial(step_kernel, (sp_count, tp_count, seq_count)),
        out_shape=[
            jax.ShapeDtypeStruct((block_rows, key_width), jnp.bfloat16),
            jax.ShapeDtypeStruct((block_rows, key_width), jnp.bfloat16),
            jax.ShapeDtypeStruct((seq_count, HEADS * VD), jnp.float32),
        ],
        in_specs=[any_space, vmem, any_space, any_space, any_space, vmem, vmem],
        out_specs=[vmem, vmem, vmem],
        scratch_shapes=[
            pltpu.VMEM((sp_count, piece_rows, width), jnp.bfloat16),
            pltpu.VMEM((2, chips, width, CORES * cols), jnp.bfloat16),
            pltpu.VMEM((width, cols), jnp.bfloat16),
            pltpu.VMEM((tp_count, 8, cols), jnp.float32),
            pltpu.VMEM((seq_count, 2 * HEADS, 2 * VD), jnp.float32),
            pltpu.VMEM((tp_count, 2 * HEADS, 2 * VD), jnp.float32),
            pltpu.VMEM((sp_count, 2 * HEADS, 2 * VD), jnp.float32),
            dma((4,)), dma((4,)), dma((sp_count,)), dma((2, chips)), dma((chips,)),
            dma((2, chips, 2)), dma((2, chips, 2)), dma((2, chips)), dma((2, chips)),
            dma((tp_count,)), dma((tp_count,)), dma((tp_count,)), dma((tp_count,)),
            dma((sp_count,)), dma((sp_count,)),
        ],
        compiler_params=pltpu.CompilerParams(
            collective_id=0, has_side_effects=True, vmem_limit_bytes=48 * 1024 * 1024
        ),
    )(
        prompt.reshape(slots, piece_rows, width),
        new_token, query_proj_matrix, key_weight, value_weight,
        jnp.broadcast_to(map_balance[:, None], (HEADS, VD)), head_gain[None, :],
    )
    shape = (1, 1, block_rows, key_width)
    return keys.reshape(shape), values.reshape(shape), read


def fits(mesh, key_weight, value_weight, prompt):
    tp_count, sp_count = mesh.shape["tp"], mesh.shape["sp"]
    seq_count, _, span_count = prompt.shape[:3]
    cols = key_weight.shape[1] // tp_count
    return (
        sp_count == 4
        and seq_count * span_count == sp_count
        and tp_count % CORES == 0
        and tp_count > CORES
        and cols % VD == 0
        and 3 * seq_count <= 8
        and key_weight.shape == value_weight.shape
    )


def solution(mesh):
    in_specs = (
        P(None, "tp", None, "sp", None, None),
        P(),
        P(None, "tp"),
        P(None, "tp"),
        P(None, "tp"),
        P(),
        P(),
    )
    out_specs = (P("sp", "tp", None, None), P("sp", "tp", None, None), P())

    def step(prompt, new_token, query_proj_matrix, key_weight, value_weight, map_balance, head_gain):
        body = fused if fits(mesh, key_weight, value_weight, prompt) else shards
        mapped = jax.shard_map(
            body, mesh=mesh, in_specs=in_specs, out_specs=out_specs, check_vma=False
        )
        return mapped(
            prompt, new_token, query_proj_matrix, key_weight, value_weight, map_balance, head_gain
        )

    return step
```

```python
import functools

import jax
import jax.numpy as jnp
from jax import lax
from jax.experimental import pallas as pl
from jax.experimental.pallas import tpu as pltpu
from jax.sharding import PartitionSpec as P

HEADS = 8
MAP_HEAD_SIZE = 64
VD = 128


norm_eps = 1e-06
far_below = -1e30


def joined(part, axis, combine):
    gathered = jax.tree.map(lambda a: lax.all_gather(a, axis), part)

    def take(source):
        return jax.tree.map(lambda a: lax.dynamic_index_in_dim(a, source, 0, False), gathered)

    return lax.fori_loop(
        1, lax.axis_size(axis), lambda source, state: combine(state, take(source)), take(0)
    )


def fill_cols(source, w_piece):
    product = jnp.dot(source, w_piece, preferred_element_type=jnp.float32).astype(jnp.bfloat16)
    return product


def local_new(new_token, query_proj_matrix, key_weight, value_weight):
    return (
        jnp.dot(new_token, query_proj_matrix, preferred_element_type=jnp.float32).astype(
            jnp.bfloat16
        ),
        jnp.dot(new_token, key_weight, preferred_element_type=jnp.float32).astype(jnp.bfloat16),
        jnp.dot(new_token, value_weight, preferred_element_type=jnp.float32).astype(jnp.bfloat16),
    )


def partial_read(query_matrix_rows, key_rows, value_rows):
    logit_scores = jnp.einsum(
        "bhmd,bjhmd->bhmj", query_matrix_rows, key_rows, preferred_element_type=jnp.float32
    ) * MAP_HEAD_SIZE ** (-0.5)
    peak = jnp.max(logit_scores, axis=-1)
    weights_exp = jnp.exp(logit_scores - peak[..., None])
    totals = jnp.sum(weights_exp, axis=-1)
    weighted = jnp.einsum("bhmj,bjhe->bhme", weights_exp, value_rows.astype(jnp.float32))
    return (peak, totals, weighted)


def combine(first, second):
    peak_a, totals_a, weighted_a = first
    peak_b, totals_b, weighted_b = second
    peak = jnp.maximum(peak_a, peak_b)
    factor_a = jnp.exp(peak_a - peak)
    factor_b = jnp.exp(peak_b - peak)
    return (
        peak,
        totals_a * factor_a + totals_b * factor_b,
        weighted_a * factor_a[..., None] + weighted_b * factor_b[..., None],
    )


def shards(prompt, new_token, query_proj_matrix, key_weight, value_weight, map_balance, head_gain):
    seq_count, _, span_count, _, piece_rows, model_width = prompt.shape
    token_rows = prompt.reshape(seq_count * span_count * piece_rows, model_width)
    tp_count = lax.axis_size("tp")
    key_width = key_weight.shape[1] * tp_count
    value_width = value_weight.shape[1] * tp_count
    key_piece = lax.all_gather(key_weight, "tp", axis=1, tiled=True)
    value_piece = lax.all_gather(value_weight, "tp", axis=1, tiled=True)
    key_rows = fill_cols(token_rows, key_piece)
    value_rows = fill_cols(token_rows, value_piece)
    own_columns = local_new(new_token, query_proj_matrix, key_weight, value_weight)
    queries, new_keys, new_values = (
        lax.all_gather(own_columns[0], "tp", axis=1, tiled=True),
        lax.all_gather(own_columns[1], "tp", axis=1, tiled=True),
        lax.all_gather(own_columns[2], "tp", axis=1, tiled=True),
    )
    slot_count = seq_count * span_count
    cached_keys, cached_values = (
        lax.all_to_all(
            key_rows.reshape(slot_count, piece_rows, key_width),
            "sp",
            split_axis=0,
            concat_axis=1,
            tiled=True,
        ),
        lax.all_to_all(
            value_rows.reshape(slot_count, piece_rows, value_width),
            "sp",
            split_axis=0,
            concat_axis=1,
            tiled=True,
        ),
    )
    block_rows = cached_keys.shape[1]
    key_cache = cached_keys.reshape(1, 1, block_rows, key_width)
    value_cache = cached_values.reshape(1, 1, block_rows, value_width)
    all_queries = queries.reshape(seq_count, HEADS, 2, MAP_HEAD_SIZE)
    own_seq = lax.axis_index("sp") // span_count
    own_query = lax.dynamic_slice_in_dim(all_queries, own_seq, 1, 0)
    peak, totals, weighted = partial_read(
        own_query,
        cached_keys.reshape(1, block_rows, HEADS, 2, MAP_HEAD_SIZE),
        cached_values.reshape(1, block_rows, HEADS, VD),
    )
    chosen = jnp.arange(seq_count) == own_seq
    chosen_rows = chosen[:, None, None]
    spread = (
        jnp.where(chosen_rows, peak, far_below),
        jnp.where(chosen_rows, totals, 0.0),
        jnp.where(chosen_rows[..., None], weighted, 0.0),
    )
    merged = joined(spread, ("sp", "tp"), combine)
    own_keys = new_keys.reshape(seq_count, HEADS, 2, MAP_HEAD_SIZE)
    own_score = jnp.einsum(
        "bhmd,bhmd->bhm", all_queries, own_keys, preferred_element_type=jnp.float32
    ) * MAP_HEAD_SIZE ** (-0.5)
    own_values = new_values.astype(jnp.float32).reshape(seq_count, HEADS, VD)
    own_weighted = jnp.broadcast_to(own_values[:, :, None, :], (seq_count, HEADS, 2, VD))
    own_state = (own_score, jnp.ones_like(own_score), own_weighted)
    _, totals, weighted = combine(merged, own_state)
    heads_out = weighted / totals[..., None]
    blended = heads_out[:, :, 0] - map_balance[None, :, None] * heads_out[:, :, 1]
    normed = (
        blended
        * lax.rsqrt(jnp.mean(blended * blended, axis=-1, keepdims=True) + norm_eps)
        * head_gain
    )
    return (key_cache, value_cache, normed.reshape(seq_count, HEADS * VD))


MESH = pl.DeviceIdType.MESH
CORES = 2
PIECES = 2


def merged_states(states):
    half = VD // 2
    peaks = [a[:, VD : VD + 1] for a in states]
    totals = [a[:, VD + half : VD + half + 1] for a in states]
    peak = functools.reduce(jnp.maximum, peaks)
    factors = [jnp.exp(p - peak) for p in peaks]
    total = functools.reduce(jnp.add, [t * f for t, f in zip(totals, factors)])
    weighted = functools.reduce(jnp.add, [a[:, :VD] * f for a, f in zip(states, factors)])
    return weighted, peak, total


def packed_state(weighted, peak, total):
    lane = lax.broadcasted_iota(jnp.int32, weighted.shape, 1)
    tail = jnp.where(lane < VD // 2, peak, total)
    return jnp.concatenate([weighted, tail], axis=1)


def step_kernel(
    dims,
    prompt, token, wq_hbm, wk_hbm, wv_hbm, balance, gain,
    kout, vout, read,
    xbuf, wbuf, wq, qbuf, own, stbuf, finbuf,
    loc, pr_send, pr_recv, line_send, prim_recv, sib_send, sib_recv, xy_send, sec_recv,
    pk_send, pk_recv, st_send, st_recv, fin_send, fin_recv,
):
    sp_count, tp_count, seq_count = dims
    depth = wbuf.shape[2]
    cols = wbuf.shape[3] // CORES
    chips = tp_count // CORES
    s = lax.axis_index("sp")
    t = lax.axis_index("tp")
    z = t // CORES
    c = t % CORES
    sib = z * CORES + (1 - c)
    xs = s + 1 - 2 * (s % 2)
    ys = (s + 2) % 4
    prim = (s + s // 2) % 2
    sec = 1 - prim
    lanes = pl.ds(pl.multiple_of(c * cols, cols), cols)
    step = depth // PIECES
    half = step // 2

    loads = [
        pltpu.make_async_copy(wk_hbm, wbuf.at[0, z, :, lanes], loc.at[0]),
        pltpu.make_async_copy(wv_hbm, wbuf.at[1, z, :, lanes], loc.at[1]),
        pltpu.make_async_copy(wq_hbm, wq, loc.at[2]),
        pltpu.make_async_copy(prompt.at[s], xbuf.at[s], loc.at[3]),
    ]
    for a in loads:
        a.start()

    barrier = pltpu.get_barrier_semaphore()
    for d in range(1, sp_count):
        pl.semaphore_signal(barrier, inc=1, device_id=((s + d) % sp_count, t), device_id_type=MESH)
    for d in range(1, tp_count):
        pl.semaphore_signal(barrier, inc=1, device_id=(s, (t + d) % tp_count), device_id_type=MESH)
    pl.semaphore_wait(barrier, sp_count + tp_count - 2)

    def remote(src, dst, send, recv, dev):
        return pltpu.make_async_remote_copy(
            src_ref=src, dst_ref=dst, send_sem=send, recv_sem=recv, device_id=dev, device_id_type=MESH
        )

    def block(m, zz):
        return wbuf.at[m, zz, :, lanes]

    def piece_of(m, zz, p):
        return wbuf.at[m, zz, pl.ds(p * step, step), lanes]

    def part(m, zz, p, h):
        return wbuf.at[m, zz, pl.ds(p * step + h * half, half), lanes]

    sends = []

    def go(copy):
        copy.start()
        sends.append(copy)

    loads[0].wait()
    loads[1].wait()

    def line(direction, zz, p):
        return remote(
            piece_of(prim, zz, p), piece_of(prim, zz, p),
            line_send.at[(direction + 1) // 2, zz, p], prim_recv.at[zz, p],
            (s, t + direction * CORES),
        )

    def has_next(direction):
        return (z > 0) if direction < 0 else (z < chips - 1)

    for direction in (-1, 1):
        @pl.when(has_next(direction))
        def _(direction=direction):
            for p in range(PIECES):
                line(direction, z, p).start()

    for d in (1, 2, 3):
        p = xs if d == 1 else ys if d == 2 else 3 - s
        go(remote(prompt.at[p], xbuf.at[s], pr_send.at[d], pr_recv.at[s], (p, t)))
    for m in range(2):
        go(remote(block(m, z), block(m, z), sib_send.at[m, z, 0], sib_recv.at[m, z, 0], (s, sib)))

    loads[2].wait()
    rows = token[...]
    me_q = jnp.dot(rows, wq[...], preferred_element_type=jnp.float32)
    me_k = jnp.dot(rows, wbuf[0, z, :, lanes], preferred_element_type=jnp.float32)
    me_v = jnp.dot(rows, wbuf[1, z, :, lanes], preferred_element_type=jnp.float32)
    for i, value in enumerate((me_q, me_k, me_v)):
        value = value.astype(jnp.bfloat16).astype(jnp.float32)
        qbuf[t, i * seq_count : (i + 1) * seq_count, :] = value[:seq_count]
    for d in range(1, tp_count):
        go(remote(qbuf.at[t], qbuf.at[t], pk_send.at[d], pk_recv.at[t], (s, (t + d) % tp_count)))

    near = jnp.minimum(z, chips - 1 - z)

    def source(j):
        paired = j <= 2 * near
        dist = jnp.where(paired, (j + 1) // 2, j - near)
        from_left = jnp.where(paired, j % 2 == 1, z > near)
        return jnp.where(from_left, z - dist, z + dist), from_left

    sources = [source(j) for j in range(1, chips)]

    def forwards(from_left):
        return (
            jnp.logical_and(from_left, z < chips - 1),
            jnp.logical_and(jnp.logical_not(from_left), z > 0),
        )

    def arrive_primary(j, p):
        zz, from_left = sources[j]
        view = piece_of(prim, zz, p)
        remote(view, view, line_send.at[0, zz, p], prim_recv.at[zz, p], (s, t)).wait_recv()
        for on, direction in zip(forwards(from_left), (1, -1)):
            pl.when(on)(lambda direction=direction: line(direction, zz, p).start())
        for h, to in enumerate((xs, ys)):
            view = part(prim, zz, p, h)
            go(remote(view, view, xy_send.at[h, zz, p], sec_recv.at[h, zz, p], (to, t)))
        view = piece_of(prim, zz, p)
        go(remote(view, view, sib_send.at[0, zz, p], sib_recv.at[0, zz, p], (s, sib)))

    def arrive_secondary(j):
        zz, _ = sources[j]
        for p in range(PIECES):
            for h in range(2):
                view = part(sec, zz, p, h)
                remote(view, view, xy_send.at[h, zz, p], sec_recv.at[h, zz, p], (s, t)).wait_recv()
                i = 2 * p + h
                go(remote(view, view, sib_send.at[1, zz, i], sib_recv.at[1, zz, i], (s, sib)))

    sib_lanes = pl.ds(pl.multiple_of((1 - c) * cols, cols), cols)

    def wait_sibling(m, slot, zz, parts):
        size = depth // parts
        for i in range(parts):
            view = wbuf.at[m, zz, pl.ds(i * size, size), sib_lanes]
            remote(view, view, sib_send.at[slot, zz, i], sib_recv.at[slot, zz, i], (s, t)).wait_recv()

    def multiply(m, zz):
        weights = wbuf.at[m, zz]
        columns = pl.ds(pl.multiple_of(zz * CORES * cols, CORES * cols), CORES * cols)

        def piece(i, _):
            product = jnp.dot(
                xbuf[pl.ds(2 * i, 2)].reshape(-1, depth), weights[...], preferred_element_type=jnp.float32
            ).astype(jnp.bfloat16)
            at = pl.ds(pl.multiple_of(i * product.shape[0], product.shape[0]), product.shape[0])

            def put(out):
                out[at, columns] = product

            if isinstance(m, int):
                put((kout, vout)[m])
            else:
                pl.when(m == 0)(lambda: put(kout))
                pl.when(m == 1)(lambda: put(vout))
            return 0

        lax.fori_loop(0, sp_count // 2, piece, 0)

    def multiply_primary(j):
        zz, _ = sources[j]
        wait_sibling(prim, 0, zz, PIECES)
        multiply(prim, zz)

    def multiply_secondary(j):
        zz, _ = sources[j]
        wait_sibling(sec, 1, zz, 2 * PIECES)
        multiply(sec, zz)

    last = chips - 1
    for j in range(min(2, last)):
        for p in range(PIECES):
            arrive_primary(j, p)

    for d in range(1, tp_count):
        i = (t + d) % tp_count
        remote(qbuf.at[i], qbuf.at[i], pk_send.at[d], pk_recv.at[i], (s, t)).wait_recv()
    new = jnp.concatenate([qbuf[i] for i in range(tp_count)], axis=1)
    row = lax.broadcasted_iota(jnp.int32, (2 * HEADS, new.shape[1]), 0)
    lane = lax.broadcasted_iota(jnp.int32, (2 * HEADS, new.shape[1]), 1)
    own_lane = lane // MAP_HEAD_SIZE == (row % HEADS) * 2 + row // HEADS
    scale = MAP_HEAD_SIZE ** (-0.5)
    short_row = lax.broadcasted_iota(jnp.int32, (2 * HEADS, VD), 0) % HEADS

    def by_head(wide):
        return functools.reduce(
            jnp.add,
            [jnp.where(short_row == h, wide[:, h * VD : (h + 1) * VD], 0.0) for h in range(HEADS)],
        )

    own_seq = s // (sp_count // seq_count)
    query = jnp.zeros((2 * HEADS, new.shape[1]), jnp.float32)
    for b in range(seq_count):
        q_b = jnp.broadcast_to(new[b : b + 1], query.shape)
        k_b = jnp.broadcast_to(new[seq_count + b : seq_count + b + 1], query.shape)
        v_b = jnp.broadcast_to(new[2 * seq_count + b : 2 * seq_count + b + 1], query.shape)
        score = jnp.sum(jnp.where(own_lane, q_b * k_b, 0.0), axis=1, keepdims=True) * scale
        own[b] = packed_state(by_head(v_b), score, jnp.ones_like(score))
        query = jnp.where(own_seq == b, q_b, query)
    query = jnp.where(own_lane, query, 0.0).astype(jnp.bfloat16)

    loads[3].wait()
    for d, p in ((1, xs), (2, ys), (3, 3 - s)):
        remote(xbuf.at[p], xbuf.at[p], pr_send.at[d], pr_recv.at[p], (s, t)).wait_recv()
    for m in range(2):
        wait_sibling(m, m, z, 1)
        multiply(m, z)
    multiply_primary(0)
    for j in range(1, last):
        arrive_secondary(j - 1)
        later = range(PIECES) if j + 1 < last else ()
        for p in later:
            arrive_primary(j + 1, p)
            if p == 0:
                multiply_primary(j)
        if j + 1 == last and last < 3:
            multiply_primary(j)
        multiply_secondary(j - 1)
    if last > 2:
        multiply_primary(last - 1)
    arrive_secondary(last - 1)
    multiply_secondary(last - 1)

    scores = lax.dot_general(
        query, kout[...], (((1,), (1,)), ((), ())), preferred_element_type=jnp.float32
    ) * scale
    peak = jnp.max(scores, axis=1, keepdims=True)
    raised = jnp.exp(scores - peak)
    total = jnp.sum(raised, axis=1, keepdims=True)
    high = raised.astype(jnp.bfloat16)
    low = (raised - high.astype(jnp.float32)).astype(jnp.bfloat16)
    wide = jnp.dot(high, vout[...], preferred_element_type=jnp.float32)
    wide = wide + jnp.dot(low, vout[...], preferred_element_type=jnp.float32)
    stbuf[t] = packed_state(by_head(wide), peak, total)
    for d in range(1, tp_count):
        go(remote(stbuf.at[t], stbuf.at[t], st_send.at[d], st_recv.at[t], (s, (t + d) % tp_count)))
    for d in range(1, tp_count):
        i = (t + d) % tp_count
        remote(stbuf.at[i], stbuf.at[i], st_send.at[d], st_recv.at[i], (s, t)).wait_recv()
    finbuf[s] = packed_state(*merged_states([stbuf[i] for i in range(tp_count)]))
    for d in range(1, sp_count):
        go(remote(finbuf.at[s], finbuf.at[s], fin_send.at[d], fin_recv.at[s], ((s + d) % sp_count, t)))
    for d in range(1, sp_count):
        i = (s + d) % sp_count
        remote(finbuf.at[i], finbuf.at[i], fin_send.at[d], fin_recv.at[i], (s, t)).wait_recv()
    spans = sp_count // seq_count
    square = (HEADS, HEADS)
    diagonal = lax.broadcasted_iota(jnp.int32, square, 0) == lax.broadcasted_iota(jnp.int32, square, 1)
    second = jnp.sum(jnp.where(diagonal, balance[...], 0.0), axis=1, keepdims=True)
    for b in range(seq_count):
        weighted, _, total = merged_states([finbuf[b * spans + i] for i in range(spans)] + [own[b]])
        heads_out = weighted / total
        blended = heads_out[:HEADS] - second * heads_out[HEADS:]
        normed = (
            blended * lax.rsqrt(jnp.mean(blended * blended, axis=1, keepdims=True) + norm_eps) * gain[...]
        )
        for h in range(HEADS):
            read[b : b + 1, h * VD : (h + 1) * VD] = normed[h : h + 1]

    for p in range(PIECES):
        for direction in (-1, 1):
            pl.when(has_next(direction))(
                lambda direction=direction, p=p: line(direction, z, p).wait_send()
            )
        for zz, from_left in sources:
            for on, direction in zip(forwards(from_left), (1, -1)):
                pl.when(on)(
                    lambda direction=direction, zz=zz, p=p: line(direction, zz, p).wait_send()
                )
    for copy in sends:
        copy.wait_send()


def fused(prompt, new_token, query_proj_matrix, key_weight, value_weight, map_balance, head_gain):
    seq_count, _, span_count, _, piece_rows, width = prompt.shape
    sp_count, tp_count = lax.axis_size("sp"), lax.axis_size("tp")
    cols = key_weight.shape[1]
    slots = seq_count * span_count
    chips = tp_count // CORES
    key_width = cols * tp_count
    block_rows = sp_count * piece_rows
    any_space = pl.BlockSpec(memory_space=pltpu.HBM)
    vmem = pl.BlockSpec(memory_space=pltpu.VMEM)
    dma = pltpu.SemaphoreType.DMA
    keys, values, read = pl.pallas_call(
        functools.partial(step_kernel, (sp_count, tp_count, seq_count)),
        out_shape=[
            jax.ShapeDtypeStruct((block_rows, key_width), jnp.bfloat16),
            jax.ShapeDtypeStruct((block_rows, key_width), jnp.bfloat16),
            jax.ShapeDtypeStruct((seq_count, HEADS * VD), jnp.float32),
        ],
        in_specs=[any_space, vmem, any_space, any_space, any_space, vmem, vmem],
        out_specs=[vmem, vmem, vmem],
        scratch_shapes=[
            pltpu.VMEM((sp_count, piece_rows, width), jnp.bfloat16),
            pltpu.VMEM((2, chips, width, CORES * cols), jnp.bfloat16),
            pltpu.VMEM((width, cols), jnp.bfloat16),
            pltpu.VMEM((tp_count, 8, cols), jnp.float32),
            pltpu.VMEM((seq_count, 2 * HEADS, 2 * VD), jnp.float32),
            pltpu.VMEM((tp_count, 2 * HEADS, 2 * VD), jnp.float32),
            pltpu.VMEM((sp_count, 2 * HEADS, 2 * VD), jnp.float32),
            dma((4,)), dma((4,)), dma((sp_count,)), dma((2, chips, PIECES)), dma((chips, PIECES)),
            dma((2, chips, 2 * PIECES)), dma((2, chips, 2 * PIECES)),
            dma((2, chips, PIECES)), dma((2, chips, PIECES)),
            dma((tp_count,)), dma((tp_count,)), dma((tp_count,)), dma((tp_count,)),
            dma((sp_count,)), dma((sp_count,)),
        ],
        compiler_params=pltpu.CompilerParams(
            collective_id=0, has_side_effects=True, vmem_limit_bytes=62 * 1024 * 1024
        ),
    )(
        prompt.reshape(slots, piece_rows, width),
        new_token, query_proj_matrix, key_weight, value_weight,
        map_balance[None, :], head_gain[None, :],
    )
    shape = (1, 1, block_rows, key_width)
    return keys.reshape(shape), values.reshape(shape), read


def fits(mesh, key_weight, value_weight, prompt):
    tp_count, sp_count = mesh.shape["tp"], mesh.shape["sp"]
    seq_count, _, span_count = prompt.shape[:3]
    cols = key_weight.shape[1] // tp_count
    return (
        sp_count == 4
        and seq_count * span_count == sp_count
        and tp_count % CORES == 0
        and tp_count > CORES
        and cols % VD == 0
        and 3 * seq_count <= 8
        and key_weight.shape == value_weight.shape
    )


def solution(mesh):
    in_specs = (
        P(None, "tp", None, "sp", None, None),
        P(),
        P(None, "tp"),
        P(None, "tp"),
        P(None, "tp"),
        P(),
        P(),
    )
    out_specs = (P("sp", "tp", None, None), P("sp", "tp", None, None), P())

    def step(prompt, new_token, query_proj_matrix, key_weight, value_weight, map_balance, head_gain):
        body = fused if fits(mesh, key_weight, value_weight, prompt) else shards
        mapped = jax.shard_map(
            body, mesh=mesh, in_specs=in_specs, out_specs=out_specs, check_vma=False
        )
        return mapped(
            prompt, new_token, query_proj_matrix, key_weight, value_weight, map_balance, head_gain
        )

    return step
```

```python
import functools

import jax
import jax.numpy as jnp
from jax import lax
from jax.experimental import pallas as pl
from jax.experimental.pallas import tpu as pltpu
from jax.sharding import PartitionSpec as P

HEADS = 8
MAP_HEAD_SIZE = 64
VD = 128


norm_eps = 1e-06
far_below = -1e30


def joined(part, axis, combine):
    gathered = jax.tree.map(lambda a: lax.all_gather(a, axis), part)

    def take(source):
        return jax.tree.map(lambda a: lax.dynamic_index_in_dim(a, source, 0, False), gathered)

    return lax.fori_loop(
        1, lax.axis_size(axis), lambda source, state: combine(state, take(source)), take(0)
    )


def fill_cols(source, w_piece):
    product = jnp.dot(source, w_piece, preferred_element_type=jnp.float32).astype(jnp.bfloat16)
    return product


def local_new(new_token, query_proj_matrix, key_weight, value_weight):
    return (
        jnp.dot(new_token, query_proj_matrix, preferred_element_type=jnp.float32).astype(
            jnp.bfloat16
        ),
        jnp.dot(new_token, key_weight, preferred_element_type=jnp.float32).astype(jnp.bfloat16),
        jnp.dot(new_token, value_weight, preferred_element_type=jnp.float32).astype(jnp.bfloat16),
    )


def partial_read(query_matrix_rows, key_rows, value_rows):
    logit_scores = jnp.einsum(
        "bhmd,bjhmd->bhmj", query_matrix_rows, key_rows, preferred_element_type=jnp.float32
    ) * MAP_HEAD_SIZE ** (-0.5)
    peak = jnp.max(logit_scores, axis=-1)
    weights_exp = jnp.exp(logit_scores - peak[..., None])
    totals = jnp.sum(weights_exp, axis=-1)
    weighted = jnp.einsum("bhmj,bjhe->bhme", weights_exp, value_rows.astype(jnp.float32))
    return (peak, totals, weighted)


def combine(first, second):
    peak_a, totals_a, weighted_a = first
    peak_b, totals_b, weighted_b = second
    peak = jnp.maximum(peak_a, peak_b)
    factor_a = jnp.exp(peak_a - peak)
    factor_b = jnp.exp(peak_b - peak)
    return (
        peak,
        totals_a * factor_a + totals_b * factor_b,
        weighted_a * factor_a[..., None] + weighted_b * factor_b[..., None],
    )


def shards(prompt, new_token, query_proj_matrix, key_weight, value_weight, map_balance, head_gain):
    seq_count, _, span_count, _, piece_rows, model_width = prompt.shape
    token_rows = prompt.reshape(seq_count * span_count * piece_rows, model_width)
    tp_count = lax.axis_size("tp")
    key_width = key_weight.shape[1] * tp_count
    value_width = value_weight.shape[1] * tp_count
    key_piece = lax.all_gather(key_weight, "tp", axis=1, tiled=True)
    value_piece = lax.all_gather(value_weight, "tp", axis=1, tiled=True)
    key_rows = fill_cols(token_rows, key_piece)
    value_rows = fill_cols(token_rows, value_piece)
    own_columns = local_new(new_token, query_proj_matrix, key_weight, value_weight)
    queries, new_keys, new_values = (
        lax.all_gather(own_columns[0], "tp", axis=1, tiled=True),
        lax.all_gather(own_columns[1], "tp", axis=1, tiled=True),
        lax.all_gather(own_columns[2], "tp", axis=1, tiled=True),
    )
    slot_count = seq_count * span_count
    cached_keys, cached_values = (
        lax.all_to_all(
            key_rows.reshape(slot_count, piece_rows, key_width),
            "sp",
            split_axis=0,
            concat_axis=1,
            tiled=True,
        ),
        lax.all_to_all(
            value_rows.reshape(slot_count, piece_rows, value_width),
            "sp",
            split_axis=0,
            concat_axis=1,
            tiled=True,
        ),
    )
    block_rows = cached_keys.shape[1]
    key_cache = cached_keys.reshape(1, 1, block_rows, key_width)
    value_cache = cached_values.reshape(1, 1, block_rows, value_width)
    all_queries = queries.reshape(seq_count, HEADS, 2, MAP_HEAD_SIZE)
    own_seq = lax.axis_index("sp") // span_count
    own_query = lax.dynamic_slice_in_dim(all_queries, own_seq, 1, 0)
    peak, totals, weighted = partial_read(
        own_query,
        cached_keys.reshape(1, block_rows, HEADS, 2, MAP_HEAD_SIZE),
        cached_values.reshape(1, block_rows, HEADS, VD),
    )
    chosen = jnp.arange(seq_count) == own_seq
    chosen_rows = chosen[:, None, None]
    spread = (
        jnp.where(chosen_rows, peak, far_below),
        jnp.where(chosen_rows, totals, 0.0),
        jnp.where(chosen_rows[..., None], weighted, 0.0),
    )
    merged = joined(spread, ("sp", "tp"), combine)
    own_keys = new_keys.reshape(seq_count, HEADS, 2, MAP_HEAD_SIZE)
    own_score = jnp.einsum(
        "bhmd,bhmd->bhm", all_queries, own_keys, preferred_element_type=jnp.float32
    ) * MAP_HEAD_SIZE ** (-0.5)
    own_values = new_values.astype(jnp.float32).reshape(seq_count, HEADS, VD)
    own_weighted = jnp.broadcast_to(own_values[:, :, None, :], (seq_count, HEADS, 2, VD))
    own_state = (own_score, jnp.ones_like(own_score), own_weighted)
    _, totals, weighted = combine(merged, own_state)
    heads_out = weighted / totals[..., None]
    blended = heads_out[:, :, 0] - map_balance[None, :, None] * heads_out[:, :, 1]
    normed = (
        blended
        * lax.rsqrt(jnp.mean(blended * blended, axis=-1, keepdims=True) + norm_eps)
        * head_gain
    )
    return (key_cache, value_cache, normed.reshape(seq_count, HEADS * VD))


MESH = pl.DeviceIdType.MESH
CORES = 2
PIECES = 2


def merged_states(states):
    half = VD // 2
    peaks = [a[:, VD : VD + 1] for a in states]
    totals = [a[:, VD + half : VD + half + 1] for a in states]
    peak = functools.reduce(jnp.maximum, peaks)
    factors = [jnp.exp(p - peak) for p in peaks]
    total = functools.reduce(jnp.add, [t * f for t, f in zip(totals, factors)])
    weighted = functools.reduce(jnp.add, [a[:, :VD] * f for a, f in zip(states, factors)])
    return weighted, peak, total


def packed_state(weighted, peak, total):
    lane = lax.broadcasted_iota(jnp.int32, weighted.shape, 1)
    tail = jnp.where(lane < VD // 2, peak, total)
    return jnp.concatenate([weighted, tail], axis=1)


def step_kernel(
    dims,
    prompt, token, wq_hbm, wk_hbm, wv_hbm, balance, gain,
    kout, vout, read,
    xbuf, wbuf, wq, qbuf, own, stbuf, finbuf,
    loc, pr_send, pr_recv, line_send, prim_recv, sib_send, sib_recv, xy_send, sec_recv,
    pk_send, pk_recv, st_send, st_recv, fin_send, fin_recv,
):
    sp_count, tp_count, seq_count = dims
    depth = wbuf.shape[2]
    cols = wbuf.shape[3] // CORES
    chips = tp_count // CORES
    s = lax.axis_index("sp")
    t = lax.axis_index("tp")
    z = t // CORES
    c = t % CORES
    sib = z * CORES + (1 - c)
    xs = s + 1 - 2 * (s % 2)
    ys = (s + 2) % 4
    prim = (s + s // 2) % 2
    sec = 1 - prim
    lanes = pl.ds(pl.multiple_of(c * cols, cols), cols)
    step = depth // PIECES
    half = step // 2

    loads = [
        pltpu.make_async_copy(wk_hbm, wbuf.at[0, z, :, lanes], loc.at[0]),
        pltpu.make_async_copy(wv_hbm, wbuf.at[1, z, :, lanes], loc.at[1]),
        pltpu.make_async_copy(wq_hbm, wq, loc.at[2]),
        pltpu.make_async_copy(prompt.at[s], xbuf.at[s], loc.at[3]),
    ]
    for a in loads:
        a.start()

    barrier = pltpu.get_barrier_semaphore()
    for d in range(1, sp_count):
        pl.semaphore_signal(barrier, inc=1, device_id=((s + d) % sp_count, t), device_id_type=MESH)
    for d in range(1, tp_count):
        pl.semaphore_signal(barrier, inc=1, device_id=(s, (t + d) % tp_count), device_id_type=MESH)
    pl.semaphore_wait(barrier, sp_count + tp_count - 2)

    def remote(src, dst, send, recv, dev):
        return pltpu.make_async_remote_copy(
            src_ref=src, dst_ref=dst, send_sem=send, recv_sem=recv, device_id=dev, device_id_type=MESH
        )

    def block(m, zz):
        return wbuf.at[m, zz, :, lanes]

    def piece_of(m, zz, p):
        return wbuf.at[m, zz, pl.ds(p * step, step), lanes]

    def part(m, zz, p, h):
        return wbuf.at[m, zz, pl.ds(p * step + h * half, half), lanes]

    sends = []

    def go(copy):
        copy.start()
        sends.append(copy)

    loads[0].wait()
    loads[1].wait()

    def line(direction, zz, p):
        return remote(
            piece_of(prim, zz, p), piece_of(prim, zz, p),
            line_send.at[(direction + 1) // 2, zz, p], prim_recv.at[zz, p],
            (s, t + direction * CORES),
        )

    def has_next(direction):
        return (z > 0) if direction < 0 else (z < chips - 1)

    for direction in (-1, 1):
        @pl.when(has_next(direction))
        def _(direction=direction):
            for p in range(PIECES):
                line(direction, z, p).start()

    for d in (1, 2, 3):
        p = xs if d == 1 else ys if d == 2 else 3 - s
        go(remote(prompt.at[p], xbuf.at[s], pr_send.at[d], pr_recv.at[s], (p, t)))
    for m in range(2):
        go(remote(block(m, z), block(m, z), sib_send.at[m, z, 0], sib_recv.at[m, z, 0], (s, sib)))

    loads[2].wait()
    rows = token[...]
    me_q = jnp.dot(rows, wq[...], preferred_element_type=jnp.float32)
    me_k = jnp.dot(rows, wbuf[0, z, :, lanes], preferred_element_type=jnp.float32)
    me_v = jnp.dot(rows, wbuf[1, z, :, lanes], preferred_element_type=jnp.float32)
    for i, value in enumerate((me_q, me_k, me_v)):
        value = value.astype(jnp.bfloat16).astype(jnp.float32)
        qbuf[t, i * seq_count : (i + 1) * seq_count, :] = value[:seq_count]
    for d in range(1, tp_count):
        go(remote(qbuf.at[t], qbuf.at[t], pk_send.at[d], pk_recv.at[t], (s, (t + d) % tp_count)))

    near = jnp.minimum(z, chips - 1 - z)

    def source(j):
        paired = j <= 2 * near
        dist = jnp.where(paired, (j + 1) // 2, j - near)
        from_left = jnp.where(paired, j % 2 == 1, z > near)
        return jnp.where(from_left, z - dist, z + dist), from_left

    sources = [source(j) for j in range(1, chips)]

    def forwards(from_left):
        return (
            jnp.logical_and(from_left, z < chips - 1),
            jnp.logical_and(jnp.logical_not(from_left), z > 0),
        )

    def primary_copies(j, p):
        zz, _ = sources[j]
        copies = []
        for h, to in enumerate((xs, ys)):
            view = part(prim, zz, p, h)
            copies.append(remote(view, view, xy_send.at[h, zz, p], sec_recv.at[h, zz, p], (to, t)))
        view = piece_of(prim, zz, p)
        copies.append(remote(view, view, sib_send.at[0, zz, p], sib_recv.at[0, zz, p], (s, sib)))
        return copies

    def arrive_primary(j, p):
        zz, from_left = sources[j]
        view = piece_of(prim, zz, p)
        remote(view, view, line_send.at[0, zz, p], prim_recv.at[zz, p], (s, t)).wait_recv()
        for on, direction in zip(forwards(from_left), (1, -1)):
            pl.when(on)(lambda direction=direction: line(direction, zz, p).start())
        for copy in primary_copies(j, p):
            copy.start()

    def arrive_secondary(j):
        zz, _ = sources[j]
        for p in range(PIECES):
            for h in range(2):
                view = part(sec, zz, p, h)
                remote(view, view, xy_send.at[h, zz, p], sec_recv.at[h, zz, p], (s, t)).wait_recv()
                i = 2 * p + h
                go(remote(view, view, sib_send.at[1, zz, i], sib_recv.at[1, zz, i], (s, sib)))

    sib_lanes = pl.ds(pl.multiple_of((1 - c) * cols, cols), cols)

    def wait_sibling(m, slot, zz, parts):
        size = depth // parts
        for i in range(parts):
            view = wbuf.at[m, zz, pl.ds(i * size, size), sib_lanes]
            remote(view, view, sib_send.at[slot, zz, i], sib_recv.at[slot, zz, i], (s, t)).wait_recv()

    def multiply(m, zz):
        weights = wbuf.at[m, zz]
        columns = pl.ds(pl.multiple_of(zz * CORES * cols, CORES * cols), CORES * cols)

        def piece(i, _):
            product = jnp.dot(
                xbuf[pl.ds(2 * i, 2)].reshape(-1, depth), weights[...], preferred_element_type=jnp.float32
            ).astype(jnp.bfloat16)
            at = pl.ds(pl.multiple_of(i * product.shape[0], product.shape[0]), product.shape[0])

            def put(out):
                out[at, columns] = product

            if isinstance(m, int):
                put((kout, vout)[m])
            else:
                pl.when(m == 0)(lambda: put(kout))
                pl.when(m == 1)(lambda: put(vout))
            return 0

        lax.fori_loop(0, sp_count // 2, piece, 0)

    def multiply_primary(j):
        zz, _ = sources[j]
        wait_sibling(prim, 0, zz, PIECES)
        multiply(prim, zz)

    def multiply_secondary(j):
        zz, _ = sources[j]
        wait_sibling(sec, 1, zz, 2 * PIECES)
        multiply(sec, zz)

    last = chips - 1
    for j in range(min(2, last)):
        for p in range(PIECES):
            arrive_primary(j, p)
    inside = near > 0

    @pl.when(inside)
    def _():
        for j in range(2, last):
            for p in range(PIECES):
                arrive_primary(j, p)

    for d in range(1, tp_count):
        i = (t + d) % tp_count
        remote(qbuf.at[i], qbuf.at[i], pk_send.at[d], pk_recv.at[i], (s, t)).wait_recv()
    new = jnp.concatenate([qbuf[i] for i in range(tp_count)], axis=1)
    row = lax.broadcasted_iota(jnp.int32, (2 * HEADS, new.shape[1]), 0)
    lane = lax.broadcasted_iota(jnp.int32, (2 * HEADS, new.shape[1]), 1)
    own_lane = lane // MAP_HEAD_SIZE == (row % HEADS) * 2 + row // HEADS
    scale = MAP_HEAD_SIZE ** (-0.5)
    short_row = lax.broadcasted_iota(jnp.int32, (2 * HEADS, VD), 0) % HEADS

    def by_head(wide):
        return functools.reduce(
            jnp.add,
            [jnp.where(short_row == h, wide[:, h * VD : (h + 1) * VD], 0.0) for h in range(HEADS)],
        )

    own_seq = s // (sp_count // seq_count)
    query = jnp.zeros((2 * HEADS, new.shape[1]), jnp.float32)
    for b in range(seq_count):
        q_b = jnp.broadcast_to(new[b : b + 1], query.shape)
        k_b = jnp.broadcast_to(new[seq_count + b : seq_count + b + 1], query.shape)
        v_b = jnp.broadcast_to(new[2 * seq_count + b : 2 * seq_count + b + 1], query.shape)
        score = jnp.sum(jnp.where(own_lane, q_b * k_b, 0.0), axis=1, keepdims=True) * scale
        own[b] = packed_state(by_head(v_b), score, jnp.ones_like(score))
        query = jnp.where(own_seq == b, q_b, query)
    query = jnp.where(own_lane, query, 0.0).astype(jnp.bfloat16)

    loads[3].wait()
    for d, p in ((1, xs), (2, ys), (3, 3 - s)):
        remote(xbuf.at[p], xbuf.at[p], pr_send.at[d], pr_recv.at[p], (s, t)).wait_recv()
    for m in range(2):
        wait_sibling(m, m, z, 1)
        multiply(m, z)
    multiply_primary(0)
    for j in range(1, last):
        arrive_secondary(j - 1)
        later = range(PIECES) if j + 1 < last else ()
        for p in later:
            pl.when(jnp.logical_not(inside))(lambda: arrive_primary(j + 1, p))
            if p == 0:
                multiply_primary(j)
        if j + 1 == last and last < 3:
            multiply_primary(j)
        multiply_secondary(j - 1)
    if last > 2:
        multiply_primary(last - 1)
    arrive_secondary(last - 1)
    multiply_secondary(last - 1)

    scores = lax.dot_general(
        query, kout[...], (((1,), (1,)), ((), ())), preferred_element_type=jnp.float32
    ) * scale
    peak = jnp.max(scores, axis=1, keepdims=True)
    raised = jnp.exp(scores - peak)
    total = jnp.sum(raised, axis=1, keepdims=True)
    high = raised.astype(jnp.bfloat16)
    low = (raised - high.astype(jnp.float32)).astype(jnp.bfloat16)
    wide = jnp.dot(high, vout[...], preferred_element_type=jnp.float32)
    wide = wide + jnp.dot(low, vout[...], preferred_element_type=jnp.float32)
    stbuf[t] = packed_state(by_head(wide), peak, total)
    for d in range(1, tp_count):
        go(remote(stbuf.at[t], stbuf.at[t], st_send.at[d], st_recv.at[t], (s, (t + d) % tp_count)))
    for d in range(1, tp_count):
        i = (t + d) % tp_count
        remote(stbuf.at[i], stbuf.at[i], st_send.at[d], st_recv.at[i], (s, t)).wait_recv()
    finbuf[s] = packed_state(*merged_states([stbuf[i] for i in range(tp_count)]))
    for d in range(1, sp_count):
        go(remote(finbuf.at[s], finbuf.at[s], fin_send.at[d], fin_recv.at[s], ((s + d) % sp_count, t)))
    for d in range(1, sp_count):
        i = (s + d) % sp_count
        remote(finbuf.at[i], finbuf.at[i], fin_send.at[d], fin_recv.at[i], (s, t)).wait_recv()
    spans = sp_count // seq_count
    square = (HEADS, HEADS)
    diagonal = lax.broadcasted_iota(jnp.int32, square, 0) == lax.broadcasted_iota(jnp.int32, square, 1)
    second = jnp.sum(jnp.where(diagonal, balance[...], 0.0), axis=1, keepdims=True)
    for b in range(seq_count):
        weighted, _, total = merged_states([finbuf[b * spans + i] for i in range(spans)] + [own[b]])
        heads_out = weighted / total
        blended = heads_out[:HEADS] - second * heads_out[HEADS:]
        normed = (
            blended * lax.rsqrt(jnp.mean(blended * blended, axis=1, keepdims=True) + norm_eps) * gain[...]
        )
        for h in range(HEADS):
            read[b : b + 1, h * VD : (h + 1) * VD] = normed[h : h + 1]

    for p in range(PIECES):
        for direction in (-1, 1):
            pl.when(has_next(direction))(
                lambda direction=direction, p=p: line(direction, z, p).wait_send()
            )
        for zz, from_left in sources:
            for on, direction in zip(forwards(from_left), (1, -1)):
                pl.when(on)(
                    lambda direction=direction, zz=zz, p=p: line(direction, zz, p).wait_send()
                )
    for j in range(last):
        for p in range(PIECES):
            sends.extend(primary_copies(j, p))
    for copy in sends:
        copy.wait_send()


def fused(prompt, new_token, query_proj_matrix, key_weight, value_weight, map_balance, head_gain):
    seq_count, _, span_count, _, piece_rows, width = prompt.shape
    sp_count, tp_count = lax.axis_size("sp"), lax.axis_size("tp")
    cols = key_weight.shape[1]
    slots = seq_count * span_count
    chips = tp_count // CORES
    key_width = cols * tp_count
    block_rows = sp_count * piece_rows
    any_space = pl.BlockSpec(memory_space=pltpu.HBM)
    vmem = pl.BlockSpec(memory_space=pltpu.VMEM)
    dma = pltpu.SemaphoreType.DMA
    keys, values, read = pl.pallas_call(
        functools.partial(step_kernel, (sp_count, tp_count, seq_count)),
        out_shape=[
            pltpu.VMEM((block_rows, key_width), jnp.bfloat16),
            pltpu.VMEM((block_rows, key_width), jnp.bfloat16),
            pltpu.VMEM((seq_count, HEADS * VD), jnp.float32),
        ],
        in_specs=[any_space, vmem, any_space, any_space, any_space, vmem, vmem],
        out_specs=[vmem, vmem, vmem],
        scratch_shapes=[
            pltpu.VMEM((sp_count, piece_rows, width), jnp.bfloat16),
            pltpu.VMEM((2, chips, width, CORES * cols), jnp.bfloat16),
            pltpu.VMEM((width, cols), jnp.bfloat16),
            pltpu.VMEM((tp_count, 8, cols), jnp.float32),
            pltpu.VMEM((seq_count, 2 * HEADS, 2 * VD), jnp.float32),
            pltpu.VMEM((tp_count, 2 * HEADS, 2 * VD), jnp.float32),
            pltpu.VMEM((sp_count, 2 * HEADS, 2 * VD), jnp.float32),
            dma((4,)), dma((4,)), dma((sp_count,)), dma((2, chips, PIECES)), dma((chips, PIECES)),
            dma((2, chips, 2 * PIECES)), dma((2, chips, 2 * PIECES)),
            dma((2, chips, PIECES)), dma((2, chips, PIECES)),
            dma((tp_count,)), dma((tp_count,)), dma((tp_count,)), dma((tp_count,)),
            dma((sp_count,)), dma((sp_count,)),
        ],
        compiler_params=pltpu.CompilerParams(
            collective_id=0, has_side_effects=True, vmem_limit_bytes=61 * 1024 * 1024 + 800 * 1024
        ),
    )(
        prompt.reshape(slots, piece_rows, width),
        new_token, query_proj_matrix, key_weight, value_weight,
        map_balance[None, :], head_gain[None, :],
    )
    shape = (1, 1, block_rows, key_width)
    return keys.reshape(shape), values.reshape(shape), read


def fits(mesh, key_weight, value_weight, prompt):
    tp_count, sp_count = mesh.shape["tp"], mesh.shape["sp"]
    seq_count, _, span_count = prompt.shape[:3]
    cols = key_weight.shape[1] // tp_count
    return (
        sp_count == 4
        and seq_count * span_count == sp_count
        and tp_count % CORES == 0
        and tp_count > CORES
        and cols % VD == 0
        and 3 * seq_count <= 8
        and key_weight.shape == value_weight.shape
    )


def solution(mesh):
    in_specs = (
        P(None, "tp", None, "sp", None, None),
        P(),
        P(None, "tp"),
        P(None, "tp"),
        P(None, "tp"),
        P(),
        P(),
    )
    out_specs = (P("sp", "tp", None, None), P("sp", "tp", None, None), P())

    def step(prompt, new_token, query_proj_matrix, key_weight, value_weight, map_balance, head_gain):
        body = fused if fits(mesh, key_weight, value_weight, prompt) else shards
        mapped = jax.shard_map(
            body, mesh=mesh, in_specs=in_specs, out_specs=out_specs, check_vma=False
        )
        return mapped(
            prompt, new_token, query_proj_matrix, key_weight, value_weight, map_balance, head_gain
        )

    return step
```
